512 devices in a mesh: pp: 16 (over z), fs: 4 (over y), tp: 8 (over x, core).
Axes of the slice: x: 4, y: 4, z: 16, core: 2. Of those that a mesh axis runs over, the one named last changes fastest.
Arguments:
- tokens: bfloat16 [16, 512, 1024], P('pp', 'fs', 'tp'), parts along dimension 1, may hold values from -640 to 640
- query_matrix: bfloat16 [16, 1024, 1024], P('pp', None, 'tp'), may hold values from -0.1875 to 0.1875
- key_matrix: bfloat16 [16, 1024, 1024], P('pp', None, 'tp'), may hold values from -0.1875 to 0.1875
- value_matrix: bfloat16 [16, 1024, 1024], P('pp', None, 'tp'), may hold values from -0.1875 to 0.1875
- output_gate_weight: bfloat16 [16, 1024, 1024], P('pp', None, 'tp'), may hold values from -0.1875 to 0.1875
- strength_weight: bfloat16 [16, 1024, 8], P('pp', None, 'tp'), may hold values from -0.1875 to 0.1875
- decay_input_weight: bfloat16 [16, 1024, 8], P('pp', None, 'tp'), may hold values from -0.1875 to 0.1875
- decay_scale_table: float32 [16, 8], P('pp', 'tp'), may hold values from 0.00078125 to 0.234375
- log_spike_decay: float32 [16, 128, 8], P('pp', None, 'tp'), may hold values from -2.1 to 0
- head_norm_gain: float32 [16, 1024], P('pp', 'tp'), may hold values from 0.1 to 1.9
- closing_norm_gain: float32 [1024], P('tp'), may hold values from 0.1 to 1.9
Outputs:
- normalized: bfloat16 [16, 512, 1024], P('pp', 'fs', 'tp'), parts along dimension 1
The draws below stay inside these ranges and needn't reach their ends.
There are 4 independent parts, one for each index of `fs`. The reference program is written for one: setup_inputs(seed, part) draws one part's arguments, and reference() takes and returns one part's arrays. A program takes and returns all parts, laid end to end along the dimension named above; an argument that names none is the same for every part. Nothing has to cross between parts.
All inputs are finite; a program needn't handle non-finite values.
Results may differ from the reference program's by a relative error of at most 0.012.
Values may be sent and summed in bfloat16 or wider, within the bound.
No kernel may reach another device: no remote copies, remote signals or barrier semaphores. Data moves between devices by JAX's collectives and lax.ppermute only.
A program may use at most 64 MiB of HBM per device.

```python
import math
from functools import partial
import jax
import jax.numpy as jnp
from jax import lax

D = 1024
HEAD_TOTAL = 8
HEAD_DIM = 128
BLOCK = 64
SEQUENCE_LENGTH = 128
LAYER_TOTAL = 16
MICRO = 16


spike_count = 3


def draw_tokens(key, part):
    base_key, row_key = jax.random.split(jax.random.fold_in(key, 17), 2)
    column_ramp = jnp.exp(math.log(10.0) * jnp.arange(D, dtype=jnp.float32) / (D - 1))
    base_values = jnp.clip(jax.random.normal(base_key, (MICRO, SEQUENCE_LENGTH, D), jnp.float32), -4.0, 4.0)
    row_scale = jnp.exp(jax.random.uniform(row_key, (MICRO, SEQUENCE_LENGTH, 1), jnp.float32, 0.0, math.log(10.0)))
    return (base_values * row_scale * column_ramp).astype(jnp.bfloat16)


def draw_decay_scale_table(key, part):
    lower_rate = 0.3 / SEQUENCE_LENGTH
    upper_rate = 30.0 / SEQUENCE_LENGTH
    logged = jax.random.uniform(jax.random.fold_in(key, 23), (LAYER_TOTAL, HEAD_TOTAL), jnp.float32, math.log(lower_rate), math.log(upper_rate))
    return jnp.exp(logged)


def draw_log_spike_decay(key, part):
    position_random_key, layer_random_key = jax.random.split(jax.random.fold_in(key, 29))
    position_indices = jax.random.randint(position_random_key, (LAYER_TOTAL, spike_count, HEAD_TOTAL), 0, SEQUENCE_LENGTH)
    layer_indices = jnp.log(jax.random.uniform(layer_random_key, (LAYER_TOTAL, spike_count, HEAD_TOTAL), jnp.float32, 0.5, 0.8))
    hit_mask = (position_indices[:, :, None, :] == jnp.arange(SEQUENCE_LENGTH)[None, None, :, None]).astype(jnp.float32)
    return jnp.sum(hit_mask * layer_indices[:, :, None, :], axis=1)


def shard_levels(own_key, extent, cuts, least, top_value):
    level = 1.0
    for dim, shards_of in cuts:
        steps = jax.random.uniform(jax.random.fold_in(jax.random.fold_in(own_key, 6), dim), (shards_of,), jnp.float32, least / len(cuts), top_value / len(cuts))
        level = level * jnp.repeat(jnp.exp(steps), extent[dim] // shards_of).reshape((-1,) + (1,) * (len(extent) - 1 - dim))
    return level


def gaussian(own_key, extent, deviation, reach, shards=(), kind=jnp.bfloat16):
    factor_of = shard_levels(own_key, extent, shards, -0.22, 0.18) if shards else 1.0
    drawn = jax.random.normal(own_key, extent, jnp.float32) * deviation * factor_of
    return jnp.minimum(jnp.maximum(drawn, -reach), reach).astype(kind)


def setup_inputs(seed: int = 0, part: int = 0) -> dict:
    splits = jax.random.split(jax.random.key(seed), 12)
    part_splits = jax.random.split(jax.random.fold_in(splits[11], part), 12)
    return {
        "tokens": draw_tokens(jax.random.fold_in(jax.random.fold_in(splits[11], part), 71), part),
        "query_matrix": gaussian(splits[1], (LAYER_TOTAL, D, HEAD_TOTAL * HEAD_DIM), D ** -0.5, 0.1875, ((0, 16), (2, 8))),
        "key_matrix": gaussian(splits[2], (LAYER_TOTAL, D, HEAD_TOTAL * HEAD_DIM), D ** -0.5, 0.1875, ((0, 16), (2, 8))),
        "value_matrix": gaussian(splits[3], (LAYER_TOTAL, D, HEAD_TOTAL * HEAD_DIM), D ** -0.5, 0.1875, ((0, 16), (2, 8))),
        "output_gate_weight": gaussian(splits[4], (LAYER_TOTAL, D, HEAD_TOTAL * HEAD_DIM), D ** -0.5, 0.1875, ((0, 16), (2, 8))),
        "strength_weight": gaussian(splits[5], (LAYER_TOTAL, D, HEAD_TOTAL), D ** -0.5, 0.1875, ((0, 16), (2, 8))),
        "decay_input_weight": gaussian(splits[6], (LAYER_TOTAL, D, HEAD_TOTAL), D ** -0.5, 0.1875, ((0, 16), (2, 8))),
        "decay_scale_table": draw_decay_scale_table(jax.random.fold_in(splits[11], 71), part),
        "log_spike_decay": draw_log_spike_decay(jax.random.fold_in(splits[11], 71), part),
        "head_norm_gain": jnp.clip(1.0 + 0.18 * jax.random.normal(splits[9], (LAYER_TOTAL, HEAD_TOTAL * HEAD_DIM), jnp.float32), 0.1, 1.9),
        "closing_norm_gain": jnp.clip(1.0 + 0.18 * jax.random.normal(splits[10], (D,), jnp.float32), 0.1, 1.9),
    }


epsilon = 1e-06

def delta_rule(queries, keys_unit, values, beta_gate, decay_logarithm):
    length, head_count, head_width = queries.shape
    value_width = values.shape[-1]
    num_blocks = length // BLOCK
    best_precision = lax.Precision.HIGHEST

    def to_blocks(tensor):
        return tensor.reshape(num_blocks, BLOCK, head_count, -1).transpose(2, 0, 1, 3)
    query_b = to_blocks(queries)
    keys_b = to_blocks(keys_unit)
    values_b = to_blocks(values)
    beta_b = beta_gate.reshape(num_blocks, BLOCK, head_count).transpose(2, 0, 1)
    decay_b = decay_logarithm.reshape(num_blocks, BLOCK, head_count).transpose(2, 0, 1)
    cumulative = jnp.cumsum(decay_b, axis=-1)
    row_ids = lax.broadcasted_iota(jnp.int32, (BLOCK, BLOCK), 0)
    col_ids = lax.broadcasted_iota(jnp.int32, (BLOCK, BLOCK), 1)
    within = jnp.where(row_ids >= col_ids, cumulative[..., :, None] - cumulative[..., None, :], -jnp.inf)
    weights = jnp.exp(within)
    keys_beta = keys_b * beta_b[..., None]
    self_term = jnp.where(row_ids > col_ids, jnp.einsum('hnik,hnjk->hnij', keys_beta, keys_b, precision=best_precision) * weights, 0.0)
    system = self_term + jnp.eye(BLOCK, dtype=self_term.dtype)
    right_side = jnp.concatenate([values_b * beta_b[..., None], keys_beta * jnp.exp(cumulative)[..., None]], axis=-1)
    solved = jax.scipy.linalg.solve_triangular(system, right_side, lower=True, unit_diagonal=True)
    update = solved[..., :value_width]
    correct = solved[..., value_width:]
    scores = jnp.einsum('hnik,hnjk->hnij', query_b, keys_b, precision=best_precision) * weights
    query_dec = query_b * jnp.exp(cumulative)[..., None]
    keys_dec = keys_b * jnp.exp(cumulative[..., -1:] - cumulative)[..., None]
    block_decay = jnp.exp(cumulative[..., -1])

    def advance(state_matrix, inputs):
        state_update, correction_term, normed_queries, normed_keys, attention_scores, decay_factor = inputs
        new_state = state_update - jnp.einsum('rna,raq->rnq', correction_term, state_matrix, precision=best_precision)
        normed_output = jnp.einsum('rna,raq->rnq', normed_queries, state_matrix, precision=best_precision) + jnp.einsum('pak,pkr->par', attention_scores, new_state, precision=best_precision)
        state_matrix = state_matrix * decay_factor[:, None, None] + jnp.einsum('fni,fnl->fil', normed_keys, new_state, precision=best_precision)
        return (state_matrix, normed_output)
    sequence_in = tuple((jnp.moveaxis(tensor, 1, 0) for tensor in (update, correct, query_dec, keys_dec, scores, block_decay)))
    initial_state = jnp.zeros((head_count, head_width, value_width), jnp.float32)
    final_state, outputs = lax.scan(advance, initial_state, sequence_in)
    return outputs.transpose(0, 2, 1, 3).reshape(length, head_count, value_width)

def merge_head_outputs(query_projected, key_projected, value_projected, gate_logits, strength_logits, decay_logits, decay_speed, spike_log_values, gain_vector):
    length = query_projected.shape[0]
    head_count = strength_logits.shape[-1]
    head_width = query_projected.shape[1] // head_count

    def normalize(projected):
        activated = jax.nn.silu(projected).reshape(length, head_count, -1)
        return activated * lax.rsqrt(lax.optimization_barrier(jnp.sum(activated * activated, axis=-1, keepdims=True)) + epsilon)
    queries = normalize(query_projected) * head_width ** (-0.5)
    keys_unit = normalize(key_projected)
    values = jax.nn.silu(value_projected).reshape(length, head_count, -1)
    beta_gate = jax.nn.sigmoid(strength_logits)
    decay_logarithm = -decay_speed[None, :] * jax.nn.softplus(decay_logits) + spike_log_values
    mixed_out = delta_rule(queries, keys_unit, values, beta_gate, decay_logarithm)
    mixed_out = mixed_out * lax.rsqrt(lax.optimization_barrier(jnp.mean(mixed_out * mixed_out, axis=-1, keepdims=True)) + epsilon) * gain_vector.reshape(head_count, -1) * jax.nn.silu(gate_logits).reshape(length, head_count, -1)
    return mixed_out.reshape(length, -1).astype(jnp.bfloat16)

def reference(tokens, query_matrix, key_matrix, value_matrix, output_gate_weight, strength_weight, decay_input_weight, decay_scale_table, log_spike_decay, head_norm_gain, closing_norm_gain):
    hidden = tokens
    for layer_number in range(LAYER_TOTAL):
        flat_rows = hidden.reshape(-1, D)
        square = flat_rows.astype(jnp.float32)
        inv_rms = lax.rsqrt(lax.optimization_barrier(jnp.mean(square * square, axis=-1, keepdims=True)) + epsilon)
        projected = [(jnp.dot(flat_rows.astype(jnp.float32), matrix[layer_number].astype(jnp.float32), preferred_element_type=jnp.float32) * inv_rms).reshape(MICRO, SEQUENCE_LENGTH, -1) for matrix in (query_matrix, key_matrix, value_matrix, output_gate_weight, strength_weight, decay_input_weight)]
        token_mixer = partial(merge_head_outputs, decay_speed=decay_scale_table[layer_number], spike_log_values=log_spike_decay[layer_number], gain_vector=head_norm_gain[layer_number])
        mixed_out = jax.vmap(token_mixer)(projected[0], projected[1], projected[2], projected[3], projected[4], projected[5])
        hidden = (hidden.astype(jnp.float32) + mixed_out.astype(jnp.float32)).astype(jnp.bfloat16)
    square = hidden.astype(jnp.float32)
    inv_rms = lax.rsqrt(lax.optimization_barrier(jnp.mean(square * square, axis=-1, keepdims=True)) + epsilon)
    return (square * inv_rms * closing_norm_gain).astype(jnp.bfloat16)
```

```python
import jax
import jax.numpy as jnp
from jax import lax
from jax.experimental import pallas as pl
from jax.experimental.pallas import tpu as pltpu
from jax.sharding import PartitionSpec as P

epsilon = 1e-06
TILE = 32


def silu(a):
    return a / (1.0 + jnp.exp(-a))


def layer_kernel(x_ref, own_ref, weight_ref, table_ref, out_ref):
    rows, model_width = x_ref.shape
    width = own_ref.shape[1]
    bf16, f32 = jnp.bfloat16, jnp.float32
    contract_lanes = (((1,), (1,)), ((), ()))
    x = x_ref[...]
    x32 = x.astype(f32)
    inv_rms = lax.rsqrt(jnp.sum(x32 * x32, axis=1, keepdims=True) * (1.0 / model_width) + epsilon)
    projected = jnp.dot(x, weight_ref[0], preferred_element_type=f32) * inv_rms
    table = table_ref[0]
    vectors = jnp.concatenate([table, jnp.zeros_like(table)], axis=0).astype(bf16)
    logits = lax.dot_general(vectors, x, contract_lanes, preferred_element_type=f32)

    row = lax.broadcasted_iota(jnp.int32, (rows, rows), 0)
    col = lax.broadcasted_iota(jnp.int32, (rows, rows), 1)

    def to_row(column):
        return jnp.sum(jnp.where(row == col, column, 0.0), axis=0, keepdims=True)

    def to_column(line):
        return jnp.sum(jnp.where(row == col, line, 0.0), axis=1, keepdims=True)

    inv_rms_row = to_row(inv_rms)
    beta_row = 1.0 / (1.0 + jnp.exp(-(logits[0:1] * inv_rms_row)))
    decay_row = logits[1:2] * inv_rms_row
    spike_row = table[2:3, :rows]
    gain_row = table[3:4, :width]
    speed_row = table[4:5, :rows]
    softplus = jnp.maximum(decay_row, 0.0) + jnp.log(1.0 + jnp.exp(-jnp.abs(decay_row)))
    g_row = spike_row - speed_row * softplus
    beta = to_column(beta_row)
    cumulative = jnp.sum(jnp.where(row >= col, g_row, 0.0), axis=1, keepdims=True)
    decay = jnp.where(row >= col, jnp.exp(jnp.minimum(cumulative - to_row(cumulative), 0.0)), 0.0)

    query = silu(projected[:, :width])
    query = query * (lax.rsqrt(jnp.sum(query * query, axis=1, keepdims=True) + epsilon) * width**-0.5)
    key = silu(projected[:, width : 2 * width])
    key = key * lax.rsqrt(jnp.sum(key * key, axis=1, keepdims=True) + epsilon)
    value = silu(projected[:, 2 * width : 3 * width]) * beta
    gate = silu(projected[:, 3 * width :])

    key16 = key.astype(bf16)
    both = jnp.concatenate([key16, query.astype(bf16)], axis=0)
    products = lax.dot_general(both, key16, contract_lanes, preferred_element_type=f32)
    scores = (products[rows:] * decay).astype(bf16)
    system = jnp.where(row > col, products[:rows] * decay * beta, 0.0)

    tiles = rows // TILE
    same_tile = row // TILE == col // TILE
    diagonal = jnp.sum(jnp.where(same_tile, system, 0.0).reshape(tiles, TILE, rows), axis=0)
    lane = lax.broadcasted_iota(jnp.int32, (TILE, rows), 1)
    sub = lax.broadcasted_iota(jnp.int32, (TILE, rows), 0)
    first_lane = lane - lane % TILE
    pieces = [
        (sub[8 * i : 8 * i + 8] == (lane % TILE)[8 * i : 8 * i + 8]).astype(f32)
        for i in range(TILE // 8)
    ]
    for j in range(TILE - 1):
        pivot = pieces[j // 8][j % 8 : j % 8 + 1]
        for i in range(j // 8, TILE // 8):
            if j % 8 == 7 and i == j // 8:
                continue
            factor = jnp.take_along_axis(
                diagonal[8 * i : 8 * i + 8], first_lane[:8] + j, axis=1, mode="promise_in_bounds"
            )
            pieces[i] = pieces[i] - factor * pivot
    tile_inverse = jnp.concatenate(pieces, axis=0)
    block_inverse = jnp.where(
        same_tile, jnp.concatenate([tile_inverse] * tiles, axis=0), 0.0
    ).astype(bf16)
    below = jnp.where(row // TILE > col // TILE, system, 0.0).astype(bf16)
    first = jnp.dot(
        block_inverse,
        jnp.concatenate([below, value.astype(bf16)], axis=1),
        preferred_element_type=f32,
    )
    coupling = first[:, :rows].astype(bf16)
    solved = first[:, rows:]
    second = jnp.dot(
        coupling,
        jnp.concatenate([coupling, solved.astype(bf16)], axis=1),
        preferred_element_type=f32,
    )
    solved = solved - second[:, rows:]
    solved = solved + jnp.dot(
        second[:, :rows].astype(bf16), solved.astype(bf16), preferred_element_type=f32
    )
    delta = jnp.dot(scores, solved.astype(bf16), preferred_element_type=f32)
    delta = delta * lax.rsqrt(jnp.sum(delta * delta, axis=1, keepdims=True) * (1.0 / width) + epsilon)
    head_out = (delta * gain_row * gate).astype(bf16)
    out_ref[...] = (own_ref[...].astype(f32) + head_out.astype(f32)).astype(bf16)


def apply_layer(layer, everything, own, weights, tables, interpret=False):
    whole = lambda i: (0, 0)
    this_layer = lambda i: (layer, 0, 0)
    return pl.pallas_call(
        layer_kernel,
        grid=(1,),
        in_specs=[
            pl.BlockSpec(everything.shape, whole),
            pl.BlockSpec(own.shape, whole),
            pl.BlockSpec((1, *weights.shape[1:]), this_layer),
            pl.BlockSpec((1, *tables.shape[1:]), this_layer),
        ],
        out_specs=pl.BlockSpec(own.shape, whole),
        out_shape=jax.ShapeDtypeStruct(own.shape, own.dtype),
        interpret=interpret,
        name="layer",
    )(everything, own, weights, tables)


def on_device(
    tokens,
    query_matrix,
    key_matrix,
    value_matrix,
    output_gate_weight,
    strength_weight,
    decay_input_weight,
    decay_scale_table,
    log_spike_decay,
    head_norm_gain,
    closing_norm_gain,
):
    model_width = query_matrix.shape[1]
    layer_total = lax.axis_size("pp")
    packed = jnp.concatenate(
        [query_matrix[0], key_matrix[0], value_matrix[0], output_gate_weight[0]], axis=1
    )
    weights = lax.all_gather(packed, "pp", axis=0)

    def line(vector):
        vector = vector.reshape(1, -1).astype(jnp.float32)
        return jnp.pad(vector, ((0, 0), (0, model_width - vector.shape[1])))

    table = jnp.concatenate(
        [
            line(strength_weight[0]),
            line(decay_input_weight[0]),
            line(log_spike_decay[0]),
            line(head_norm_gain[0]),
            jnp.broadcast_to(decay_scale_table[0], (1, model_width)),
            jnp.zeros((3, model_width), jnp.float32),
        ],
        axis=0,
    )
    tables = lax.all_gather(table, "pp", axis=0)
    own = tokens[0]
    for layer in range(layer_total):
        everything = lax.all_gather(own, "tp", axis=1, tiled=True)
        own = apply_layer(layer, everything, own, weights, tables)
    everything = lax.all_gather(own, "tp", axis=1, tiled=True).astype(jnp.float32)
    inv_rms = lax.rsqrt(jnp.mean(everything * everything, axis=1, keepdims=True) + epsilon)
    normalized = own.astype(jnp.float32) * inv_rms * closing_norm_gain[None, :]
    return normalized.astype(jnp.bfloat16)[None]


def solution(mesh):
    placed = (
        P("pp", "fs", "tp"),
        P("pp", None, "tp"),
        P("pp", None, "tp"),
        P("pp", None, "tp"),
        P("pp", None, "tp"),
        P("pp", None, "tp"),
        P("pp", None, "tp"),
        P("pp", "tp"),
        P("pp", None, "tp"),
        P("pp", "tp"),
        P("tp"),
    )
    return jax.shard_map(
        on_device, mesh=mesh, in_specs=placed, out_specs=P("pp", "fs", "tp"), check_vma=False
    )
```

```python
import jax
import jax.numpy as jnp
from jax import lax
from jax.experimental import pallas as pl
from jax.experimental.pallas import tpu as pltpu
from jax.sharding import PartitionSpec as P

epsilon = 1e-06
TILE = 32
GROUPS = (0, 1, 3, 7, 12, 16)
DIRECT = 3


def silu(a):
    return a / (1.0 + jnp.exp(-a))


def layer_kernel(x_ref, own_ref, weight_ref, table_ref, out_ref, copies_ref):
    rows, width = own_ref.shape
    parts = weight_ref.shape[0]
    part_width = weight_ref.shape[2]
    model_width = parts * part_width
    bf16, f32 = jnp.bfloat16, jnp.float32
    contract_lanes = (((1,), (1,)), ((), ()))
    x = jnp.concatenate([x_ref[i] for i in range(x_ref.shape[0])], axis=1)
    x32 = x.astype(f32)
    inv_rms = lax.rsqrt(jnp.sum(x32 * x32, axis=1, keepdims=True) * (1.0 / model_width) + epsilon)
    projected = jnp.zeros((rows, weight_ref.shape[3]), f32)
    for i in range(parts):
        projected += jnp.dot(
            x[:, i * part_width : (i + 1) * part_width],
            weight_ref[i, 0],
            preferred_element_type=f32,
        )
    projected = projected * inv_rms
    table = table_ref[0]
    vectors = jnp.concatenate([table, jnp.zeros_like(table)], axis=0).astype(bf16)
    logits = lax.dot_general(vectors, x, contract_lanes, preferred_element_type=f32)

    row = lax.broadcasted_iota(jnp.int32, (rows, rows), 0)
    col = lax.broadcasted_iota(jnp.int32, (rows, rows), 1)

    def to_row(column):
        return jnp.sum(jnp.where(row == col, column, 0.0), axis=0, keepdims=True)

    def to_column(line):
        return jnp.sum(jnp.where(row == col, line, 0.0), axis=1, keepdims=True)

    inv_rms_row = to_row(inv_rms)
    beta_row = 1.0 / (1.0 + jnp.exp(-(logits[0:1] * inv_rms_row)))
    decay_row = logits[1:2] * inv_rms_row
    spike_row = table[2:3, :rows]
    gain_row = table[3:4, :width]
    speed_row = table[4:5, :rows]
    softplus = jnp.maximum(decay_row, 0.0) + jnp.log(1.0 + jnp.exp(-jnp.abs(decay_row)))
    g_row = spike_row - speed_row * softplus
    beta = to_column(beta_row)
    cumulative = jnp.sum(jnp.where(row >= col, g_row, 0.0), axis=1, keepdims=True)
    decay = jnp.where(row >= col, jnp.exp(jnp.minimum(cumulative - to_row(cumulative), 0.0)), 0.0)

    query = silu(projected[:, :width])
    query = query * (lax.rsqrt(jnp.sum(query * query, axis=1, keepdims=True) + epsilon) * width**-0.5)
    key = silu(projected[:, width : 2 * width])
    key = key * lax.rsqrt(jnp.sum(key * key, axis=1, keepdims=True) + epsilon)
    value = silu(projected[:, 2 * width : 3 * width]) * beta
    gate = silu(projected[:, 3 * width :])

    key16 = key.astype(bf16)
    both = jnp.concatenate([key16, query.astype(bf16)], axis=0)
    products = lax.dot_general(both, key16, contract_lanes, preferred_element_type=f32)
    scores = (products[rows:] * decay).astype(bf16)
    system = jnp.where(row > col, products[:rows] * decay * beta, 0.0)

    tiles = rows // TILE
    same_tile = row // TILE == col // TILE
    diagonal = jnp.sum(jnp.where(same_tile, system, 0.0).reshape(tiles, TILE, rows), axis=0)
    lane = lax.broadcasted_iota(jnp.int32, (TILE, rows), 1)
    sub = lax.broadcasted_iota(jnp.int32, (TILE, rows), 0)
    first_lane = lane - lane % TILE
    pieces = [
        (sub[8 * i : 8 * i + 8] == (lane % TILE)[8 * i : 8 * i + 8]).astype(f32)
        for i in range(TILE // 8)
    ]
    for j in range(TILE - 1):
        pivot = pieces[j // 8][j % 8 : j % 8 + 1]
        for i in range(j // 8, TILE // 8):
            if j % 8 == 7 and i == j // 8:
                continue
            factor = jnp.take_along_axis(
                diagonal[8 * i : 8 * i + 8], first_lane[:8] + j, axis=1, mode="promise_in_bounds"
            )
            pieces[i] = pieces[i] - factor * pivot
    tile_inverse = jnp.concatenate(pieces, axis=0)
    block_inverse = jnp.where(
        same_tile, jnp.concatenate([tile_inverse] * tiles, axis=0), 0.0
    ).astype(bf16)
    below = jnp.where(row // TILE > col // TILE, system, 0.0).astype(bf16)
    first = jnp.dot(
        block_inverse,
        jnp.concatenate([below, value.astype(bf16)], axis=1),
        preferred_element_type=f32,
    )
    coupling = first[:, :rows].astype(bf16)
    solved = first[:, rows:]
    second = jnp.dot(
        coupling,
        jnp.concatenate([coupling, solved.astype(bf16)], axis=1),
        preferred_element_type=f32,
    )
    solved = solved - second[:, rows:]
    solved = solved + jnp.dot(
        second[:, :rows].astype(bf16), solved.astype(bf16), preferred_element_type=f32
    )
    delta = jnp.dot(scores, solved.astype(bf16), preferred_element_type=f32)
    delta = delta * lax.rsqrt(jnp.sum(delta * delta, axis=1, keepdims=True) * (1.0 / width) + epsilon)
    head_out = (delta * gain_row * gate).astype(bf16)
    updated = (own_ref[...].astype(f32) + head_out.astype(f32)).astype(bf16)
    out_ref[...] = updated
    for i in range(copies_ref.shape[0]):
        copies_ref[i] = updated


def apply_layer(layer, place, everything, own, weights, tables, interpret=False):
    parts, _, part_width, columns = weights.shape
    return pl.pallas_call(
        layer_kernel,
        grid=(1,),
        in_specs=[
            pl.BlockSpec(everything.shape, lambda i: (0, 0, 0)),
            pl.BlockSpec(own.shape, lambda i: (0, 0)),
            pl.BlockSpec((parts, 1, part_width, columns), lambda i: (0, place, 0, 0)),
            pl.BlockSpec((1, *tables.shape[1:]), lambda i: (layer, 0, 0)),
        ],
        out_specs=[
            pl.BlockSpec(own.shape, lambda i: (0, 0)),
            pl.BlockSpec(everything.shape, lambda i: (0, 0, 0)),
        ],
        out_shape=[
            jax.ShapeDtypeStruct(own.shape, own.dtype),
            jax.ShapeDtypeStruct(everything.shape, own.dtype),
        ],
        interpret=interpret,
        compiler_params=pltpu.CompilerParams(vmem_limit_bytes=12 * 1024 * 1024),
        name="layer",
    )(everything, own, weights, tables)


def exchange(copies, axis):
    return lax.all_to_all(copies, axis, split_axis=0, concat_axis=0, tiled=True)


def from_everyone(shard, axis):
    return exchange(jnp.broadcast_to(shard, (lax.axis_size(axis), *shard.shape)), axis)


def on_device(
    tokens,
    query_matrix,
    key_matrix,
    value_matrix,
    output_gate_weight,
    strength_weight,
    decay_input_weight,
    decay_scale_table,
    log_spike_decay,
    head_norm_gain,
    closing_norm_gain,
):
    model_width = query_matrix.shape[1]
    layer_total = lax.axis_size("pp")
    part_rows = model_width // lax.axis_size("fs")
    first_row = lax.axis_index("fs") * part_rows
    packed = jnp.concatenate(
        [
            lax.dynamic_slice_in_dim(matrix[0], first_row, part_rows, axis=0)
            for matrix in (query_matrix, key_matrix, value_matrix, output_gate_weight)
        ],
        axis=1,
    )
    def line(vector):
        vector = vector.reshape(1, -1).astype(jnp.float32)
        return jnp.pad(vector, ((0, 0), (0, model_width - vector.shape[1])))

    table = jnp.concatenate(
        [
            line(strength_weight[0]),
            line(decay_input_weight[0]),
            line(log_spike_decay[0]),
            line(head_norm_gain[0]),
            jnp.broadcast_to(decay_scale_table[0], (1, model_width)),
            jnp.zeros((3, model_width), jnp.float32),
        ],
        axis=0,
    )
    tables = lax.all_gather(table, "pp", axis=0)
    own = tokens[0]
    everything = from_everyone(own, "tp")
    quarters = lax.all_gather(packed, "pp", axis=0)
    quarters, everything, tables = lax.optimization_barrier((quarters, everything, tables))
    stored = {}
    for begin, end in zip(GROUPS[:-1], GROUPS[1:]):
        group = quarters[begin:end]
        if begin < DIRECT:
            group = from_everyone(group, "fs")
        else:
            group = lax.all_gather(group, "fs", axis=0)
        for layer in range(begin, end):
            stored[layer] = (layer - begin, group)
    for layer in range(layer_total):
        place, weights = stored[layer]
        own, copies = apply_layer(layer, place, everything, own, weights, tables)
        everything = exchange(copies, "tp")
    square = everything.astype(jnp.float32)
    row_total = jnp.sum(jnp.sum(square * square, axis=0), axis=1, keepdims=True)
    inv_rms = lax.rsqrt(row_total / model_width + epsilon)
    normalized = own.astype(jnp.float32) * inv_rms * closing_norm_gain[None, :]
    return normalized.astype(jnp.bfloat16)[None]


def solution(mesh):
    placed = (
        P("pp", "fs", "tp"),
        P("pp", None, "tp"),
        P("pp", None, "tp"),
        P("pp", None, "tp"),
        P("pp", None, "tp"),
        P("pp", None, "tp"),
        P("pp", None, "tp"),
        P("pp", "tp"),
        P("pp", None, "tp"),
        P("pp", "tp"),
        P("tp"),
    )
    return jax.shard_map(
        on_device, mesh=mesh, in_specs=placed, out_specs=P("pp", "fs", "tp"), check_vma=False
    )
```

```python
from functools import partial

import jax
import jax.numpy as jnp
from jax import lax
from jax.experimental import pallas as pl
from jax.experimental.pallas import tpu as pltpu
from jax.sharding import PartitionSpec as P

epsilon = 1e-06
TILE = 32
GROUPS = (0, 2, 7, 12, 16)
DIRECT = 2


def silu(a):
    return a / (1.0 + jnp.exp(-a))


def layer_kernel(layer, place, x_ref, own_ref, weight_ref, table_ref, out_ref, copies_ref):
    rows, width = own_ref.shape
    parts = weight_ref.shape[0]
    part_width = weight_ref.shape[2]
    model_width = parts * part_width
    bf16, f32 = jnp.bfloat16, jnp.float32
    contract_lanes = (((1,), (1,)), ((), ()))
    x = jnp.concatenate([x_ref[i] for i in range(x_ref.shape[0])], axis=1)
    x32 = x.astype(f32)
    inv_rms = lax.rsqrt(jnp.sum(x32 * x32, axis=1, keepdims=True) * (1.0 / model_width) + epsilon)
    projected = jnp.zeros((rows, weight_ref.shape[3]), f32)
    for i in range(parts):
        projected += jnp.dot(
            x[:, i * part_width : (i + 1) * part_width],
            weight_ref[i, place],
            preferred_element_type=f32,
        )
    projected = projected * inv_rms
    table = table_ref[layer]
    vectors = jnp.concatenate([table, jnp.zeros_like(table)], axis=0).astype(bf16)
    logits = lax.dot_general(vectors, x, contract_lanes, preferred_element_type=f32)

    row = lax.broadcasted_iota(jnp.int32, (rows, rows), 0)
    col = lax.broadcasted_iota(jnp.int32, (rows, rows), 1)

    def to_row(column):
        return jnp.sum(jnp.where(row == col, column, 0.0), axis=0, keepdims=True)

    def to_column(line):
        return jnp.sum(jnp.where(row == col, line, 0.0), axis=1, keepdims=True)

    inv_rms_row = to_row(inv_rms)
    beta_row = 1.0 / (1.0 + jnp.exp(-(logits[0:1] * inv_rms_row)))
    decay_row = logits[1:2] * inv_rms_row
    spike_row = table[2:3, :rows]
    gain_row = table[3:4, :width]
    speed_row = table[4:5, :rows]
    softplus = jnp.maximum(decay_row, 0.0) + jnp.log(1.0 + jnp.exp(-jnp.abs(decay_row)))
    g_row = spike_row - speed_row * softplus
    beta = to_column(beta_row)
    cumulative = jnp.sum(jnp.where(row >= col, g_row, 0.0), axis=1, keepdims=True)
    decay = jnp.where(row >= col, jnp.exp(jnp.minimum(cumulative - to_row(cumulative), 0.0)), 0.0)

    query = silu(projected[:, :width])
    query = query * (lax.rsqrt(jnp.sum(query * query, axis=1, keepdims=True) + epsilon) * width**-0.5)
    key = silu(projected[:, width : 2 * width])
    key = key * lax.rsqrt(jnp.sum(key * key, axis=1, keepdims=True) + epsilon)
    value = silu(projected[:, 2 * width : 3 * width]) * beta
    gate = silu(projected[:, 3 * width :])

    key16 = key.astype(bf16)
    both = jnp.concatenate([key16, query.astype(bf16)], axis=0)
    products = lax.dot_general(both, key16, contract_lanes, preferred_element_type=f32)
    scores = (products[rows:] * decay).astype(bf16)
    system = jnp.where(row > col, products[:rows] * decay * beta, 0.0)

    tiles = rows // TILE
    same_tile = row // TILE == col // TILE
    diagonal = jnp.sum(jnp.where(same_tile, system, 0.0).reshape(tiles, TILE, rows), axis=0)
    lane = lax.broadcasted_iota(jnp.int32, (TILE, rows), 1)
    sub = lax.broadcasted_iota(jnp.int32, (TILE, rows), 0)
    first_lane = lane - lane % TILE
    pieces = [
        (sub[8 * i : 8 * i + 8] == (lane % TILE)[8 * i : 8 * i + 8]).astype(f32)
        for i in range(TILE // 8)
    ]
    for j in range(TILE - 1):
        pivot = pieces[j // 8][j % 8 : j % 8 + 1]
        for i in range(j // 8, TILE // 8):
            if j % 8 == 7 and i == j // 8:
                continue
            factor = jnp.take_along_axis(
                diagonal[8 * i : 8 * i + 8], first_lane[:8] + j, axis=1, mode="promise_in_bounds"
            )
            pieces[i] = pieces[i] - factor * pivot
    tile_inverse = jnp.concatenate(pieces, axis=0)
    block_inverse = jnp.where(
        same_tile, jnp.concatenate([tile_inverse] * tiles, axis=0), 0.0
    ).astype(bf16)
    below = jnp.where(row // TILE > col // TILE, system, 0.0).astype(bf16)
    first = jnp.dot(
        block_inverse,
        jnp.concatenate([below, value.astype(bf16)], axis=1),
        preferred_element_type=f32,
    )
    coupling = first[:, :rows].astype(bf16)
    solved = first[:, rows:]
    second = jnp.dot(
        coupling,
        jnp.concatenate([coupling, solved.astype(bf16)], axis=1),
        preferred_element_type=f32,
    )
    solved = solved - second[:, rows:]
    solved = solved + jnp.dot(
        second[:, :rows].astype(bf16), solved.astype(bf16), preferred_element_type=f32
    )
    delta = jnp.dot(scores, solved.astype(bf16), preferred_element_type=f32)
    delta = delta * lax.rsqrt(jnp.sum(delta * delta, axis=1, keepdims=True) * (1.0 / width) + epsilon)
    head_out = (delta * gain_row * gate).astype(bf16)
    updated = (own_ref[...].astype(f32) + head_out.astype(f32)).astype(bf16)
    out_ref[...] = updated
    for i in range(copies_ref.shape[0]):
        copies_ref[i] = updated


def apply_layer(layer, place, everything, own, weights, tables, interpret=False):
    in_vmem = pl.BlockSpec(memory_space=pltpu.VMEM)
    return pl.pallas_call(
        partial(layer_kernel, layer, place),
        in_specs=[in_vmem] * 4,
        out_specs=[in_vmem] * 2,
        out_shape=[
            jax.ShapeDtypeStruct(own.shape, own.dtype),
            jax.ShapeDtypeStruct(everything.shape, own.dtype),
        ],
        interpret=interpret,
        compiler_params=pltpu.CompilerParams(vmem_limit_bytes=12 * 1024 * 1024),
        name="layer",
    )(everything, own, weights, tables)


def exchange(copies, axis):
    return lax.all_to_all(copies, axis, split_axis=0, concat_axis=0, tiled=True)


def from_everyone(shard, axis):
    return exchange(jnp.broadcast_to(shard, (lax.axis_size(axis), *shard.shape)), axis)


def on_device(
    tokens,
    query_matrix,
    key_matrix,
    value_matrix,
    output_gate_weight,
    strength_weight,
    decay_input_weight,
    decay_scale_table,
    log_spike_decay,
    head_norm_gain,
    closing_norm_gain,
):
    model_width = query_matrix.shape[1]
    layer_total = lax.axis_size("pp")
    part_rows = model_width // lax.axis_size("fs")
    first_row = lax.axis_index("fs") * part_rows
    packed = jnp.concatenate(
        [
            lax.dynamic_slice_in_dim(matrix[0], first_row, part_rows, axis=0)
            for matrix in (query_matrix, key_matrix, value_matrix, output_gate_weight)
        ],
        axis=1,
    )
    def line(vector):
        vector = vector.reshape(1, -1).astype(jnp.float32)
        return jnp.pad(vector, ((0, 0), (0, model_width - vector.shape[1])))

    table = jnp.concatenate(
        [
            line(strength_weight[0]),
            line(decay_input_weight[0]),
            line(log_spike_decay[0]),
            line(head_norm_gain[0]),
            jnp.broadcast_to(decay_scale_table[0], (1, model_width)),
            jnp.zeros((3, model_width), jnp.float32),
        ],
        axis=0,
    )
    tables = lax.all_gather(table, "pp", axis=0)
    own = tokens[0]
    everything = from_everyone(own, "tp")
    quarters = lax.all_gather(packed, "pp", axis=0)
    quarters, everything, tables = lax.optimization_barrier((quarters, everything, tables))
    stored = {}
    for begin, end in zip(GROUPS[:-1], GROUPS[1:]):
        if begin > DIRECT:
            quarters, stored[0] = lax.optimization_barrier((quarters, stored[0]))
        group = quarters[begin:end]
        if begin < DIRECT:
            group = from_everyone(group, "fs")
        else:
            group = lax.all_gather(group, "fs", axis=0)
        for layer in range(begin, end):
            stored[layer] = group
    for layer in range(layer_total):
        place = layer - max(begin for begin in GROUPS if begin <= layer)
        own, copies = apply_layer(layer, place, everything, own, stored[layer], tables)
        everything = exchange(copies, "tp")
    square = everything.astype(jnp.float32)
    row_total = jnp.sum(jnp.sum(square * square, axis=0), axis=1, keepdims=True)
    inv_rms = lax.rsqrt(row_total / model_width + epsilon)
    normalized = own.astype(jnp.float32) * inv_rms * closing_norm_gain[None, :]
    return normalized.astype(jnp.bfloat16)[None]


def solution(mesh):
    placed = (
        P("pp", "fs", "tp"),
        P("pp", None, "tp"),
        P("pp", None, "tp"),
        P("pp", None, "tp"),
        P("pp", None, "tp"),
        P("pp", None, "tp"),
        P("pp", None, "tp"),
        P("pp", "tp"),
        P("pp", None, "tp"),
        P("pp", "tp"),
        P("tp"),
    )
    return jax.shard_map(
        on_device, mesh=mesh, in_specs=placed, out_specs=P("pp", "fs", "tp"), check_vma=False
    )
```

```python
from functools import partial

import jax
import jax.numpy as jnp
from jax import lax
from jax.experimental import pallas as pl
from jax.experimental.pallas import tpu as pltpu
from jax.sharding import PartitionSpec as P

epsilon = 1e-06
TILE = 32
GROUPS = (0, 2, 7, 12, 16)
DIRECT = 2


def silu(a):
    return a / (1.0 + jnp.exp(-a))


def fetching_kernel(
    layer, place, x_ref, own_ref, remote_ref, table_ref, out_ref, copies_ref, weight_ref, sems
):
    pieces = [
        pltpu.make_async_copy(remote_ref.at[i, place], weight_ref.at[i, 0], sems.at[i])
        for i in range(remote_ref.shape[0])
    ]
    for piece in pieces:
        piece.start()
    layer_body(
        layer, 0, pieces, x_ref, own_ref, weight_ref, table_ref, out_ref, copies_ref
    )


def layer_kernel(layer, place, x_ref, own_ref, weight_ref, table_ref, out_ref, copies_ref):
    layer_body(layer, place, (), x_ref, own_ref, weight_ref, table_ref, out_ref, copies_ref)


def layer_body(
    layer, place, pieces, x_ref, own_ref, weight_ref, table_ref, out_ref, copies_ref
):
    rows, width = own_ref.shape
    parts = weight_ref.shape[0]
    part_width = weight_ref.shape[2]
    model_width = parts * part_width
    bf16, f32 = jnp.bfloat16, jnp.float32
    contract_lanes = (((1,), (1,)), ((), ()))
    x = jnp.concatenate([x_ref[i] for i in range(x_ref.shape[0])], axis=1)
    x32 = x.astype(f32)
    inv_rms = lax.rsqrt(jnp.sum(x32 * x32, axis=1, keepdims=True) * (1.0 / model_width) + epsilon)
    projected = jnp.zeros((rows, weight_ref.shape[3]), f32)
    for i in range(parts):
        if pieces:
            pieces[i].wait()
        projected += jnp.dot(
            x[:, i * part_width : (i + 1) * part_width],
            weight_ref[i, place],
            preferred_element_type=f32,
        )
    projected = projected * inv_rms
    table = table_ref[layer]
    vectors = jnp.concatenate([table, jnp.zeros_like(table)], axis=0).astype(bf16)
    logits = lax.dot_general(vectors, x, contract_lanes, preferred_element_type=f32)

    row = lax.broadcasted_iota(jnp.int32, (rows, rows), 0)
    col = lax.broadcasted_iota(jnp.int32, (rows, rows), 1)

    def to_row(column):
        return jnp.sum(jnp.where(row == col, column, 0.0), axis=0, keepdims=True)

    def to_column(line):
        return jnp.sum(jnp.where(row == col, line, 0.0), axis=1, keepdims=True)

    inv_rms_row = to_row(inv_rms)
    beta_row = 1.0 / (1.0 + jnp.exp(-(logits[0:1] * inv_rms_row)))
    decay_row = logits[1:2] * inv_rms_row
    spike_row = table[2:3, :rows]
    gain_row = table[3:4, :width]
    speed_row = table[4:5, :rows]
    softplus = jnp.maximum(decay_row, 0.0) + jnp.log(1.0 + jnp.exp(-jnp.abs(decay_row)))
    g_row = spike_row - speed_row * softplus
    beta = to_column(beta_row)
    cumulative = jnp.sum(jnp.where(row >= col, g_row, 0.0), axis=1, keepdims=True)
    decay = jnp.where(row >= col, jnp.exp(jnp.minimum(cumulative - to_row(cumulative), 0.0)), 0.0)

    query = silu(projected[:, :width])
    query = query * (lax.rsqrt(jnp.sum(query * query, axis=1, keepdims=True) + epsilon) * width**-0.5)
    key = silu(projected[:, width : 2 * width])
    key = key * lax.rsqrt(jnp.sum(key * key, axis=1, keepdims=True) + epsilon)
    value = silu(projected[:, 2 * width : 3 * width]) * beta
    gate = silu(projected[:, 3 * width :])

    key16 = key.astype(bf16)
    both = jnp.concatenate([key16, query.astype(bf16)], axis=0)
    products = lax.dot_general(both, key16, contract_lanes, preferred_element_type=f32)
    scores = (products[rows:] * decay).astype(bf16)
    system = jnp.where(row > col, products[:rows] * decay * beta, 0.0)

    tiles = rows // TILE
    same_tile = row // TILE == col // TILE
    diagonal = jnp.sum(jnp.where(same_tile, system, 0.0).reshape(tiles, TILE, rows), axis=0)
    lane = lax.broadcasted_iota(jnp.int32, (TILE, rows), 1)
    sub = lax.broadcasted_iota(jnp.int32, (TILE, rows), 0)
    first_lane = lane - lane % TILE
    pieces = [
        (sub[8 * i : 8 * i + 8] == (lane % TILE)[8 * i : 8 * i + 8]).astype(f32)
        for i in range(TILE // 8)
    ]
    for j in range(TILE - 1):
        pivot = pieces[j // 8][j % 8 : j % 8 + 1]
        for i in range(j // 8, TILE // 8):
            if j % 8 == 7 and i == j // 8:
                continue
            factor = jnp.take_along_axis(
                diagonal[8 * i : 8 * i + 8], first_lane[:8] + j, axis=1, mode="promise_in_bounds"
            )
            pieces[i] = pieces[i] - factor * pivot
    tile_inverse = jnp.concatenate(pieces, axis=0)
    block_inverse = jnp.where(
        same_tile, jnp.concatenate([tile_inverse] * tiles, axis=0), 0.0
    ).astype(bf16)
    below = jnp.where(row // TILE > col // TILE, system, 0.0).astype(bf16)
    first = jnp.dot(
        block_inverse,
        jnp.concatenate([below, value.astype(bf16)], axis=1),
        preferred_element_type=f32,
    )
    coupling = first[:, :rows].astype(bf16)
    solved = first[:, rows:]
    second = jnp.dot(
        coupling,
        jnp.concatenate([coupling, solved.astype(bf16)], axis=1),
        preferred_element_type=f32,
    )
    solved = solved - second[:, rows:]
    solved = solved + jnp.dot(
        second[:, :rows].astype(bf16), solved.astype(bf16), preferred_element_type=f32
    )
    delta = jnp.dot(scores, solved.astype(bf16), preferred_element_type=f32)
    delta = delta * lax.rsqrt(jnp.sum(delta * delta, axis=1, keepdims=True) * (1.0 / width) + epsilon)
    head_out = (delta * gain_row * gate).astype(bf16)
    updated = (own_ref[...].astype(f32) + head_out.astype(f32)).astype(bf16)
    out_ref[...] = updated
    for i in range(copies_ref.shape[0]):
        copies_ref[i] = updated


def apply_layer(layer, place, fetch, everything, own, weights, tables, interpret=False):
    in_vmem = pl.BlockSpec(memory_space=pltpu.VMEM)
    anywhere = pl.BlockSpec(memory_space=pltpu.HBM)
    parts, _, part_width, columns = weights.shape
    scratch = [
        pltpu.VMEM((parts, 1, part_width, columns), weights.dtype),
        pltpu.SemaphoreType.DMA((parts,)),
    ]
    return pl.pallas_call(
        partial(fetching_kernel if fetch else layer_kernel, layer, place),
        scratch_shapes=scratch if fetch else [],
        in_specs=[in_vmem, in_vmem, anywhere if fetch else in_vmem, in_vmem],
        out_specs=[in_vmem] * 2,
        out_shape=[
            jax.ShapeDtypeStruct(own.shape, own.dtype),
            jax.ShapeDtypeStruct(everything.shape, own.dtype),
        ],
        interpret=interpret,
        compiler_params=pltpu.CompilerParams(vmem_limit_bytes=12 * 1024 * 1024),
        name="layer",
    )(everything, own, weights, tables)


def exchange(copies, axis):
    return lax.all_to_all(copies, axis, split_axis=0, concat_axis=0, tiled=True)


def from_everyone(shard, axis):
    return exchange(jnp.broadcast_to(shard, (lax.axis_size(axis), *shard.shape)), axis)


def on_device(
    tokens,
    query_matrix,
    key_matrix,
    value_matrix,
    output_gate_weight,
    strength_weight,
    decay_input_weight,
    decay_scale_table,
    log_spike_decay,
    head_norm_gain,
    closing_norm_gain,
):
    model_width = query_matrix.shape[1]
    layer_total = lax.axis_size("pp")
    part_rows = model_width // lax.axis_size("fs")
    first_row = lax.axis_index("fs") * part_rows
    packed = jnp.concatenate(
        [
            lax.dynamic_slice_in_dim(matrix[0], first_row, part_rows, axis=0)
            for matrix in (query_matrix, key_matrix, value_matrix, output_gate_weight)
        ],
        axis=1,
    )
    def line(vector):
        vector = vector.reshape(1, -1).astype(jnp.float32)
        return jnp.pad(vector, ((0, 0), (0, model_width - vector.shape[1])))

    table = jnp.concatenate(
        [
            line(strength_weight[0]),
            line(decay_input_weight[0]),
            line(log_spike_decay[0]),
            line(head_norm_gain[0]),
            jnp.broadcast_to(decay_scale_table[0], (1, model_width)),
            jnp.zeros((3, model_width), jnp.float32),
        ],
        axis=0,
    )
    tables = lax.all_gather(table, "pp", axis=0)
    own = tokens[0]
    everything = from_everyone(own, "tp")
    quarters = lax.all_gather(packed, "pp", axis=0)
    quarters, everything, tables = lax.optimization_barrier((quarters, everything, tables))
    stored = {}
    for begin, end in zip(GROUPS[:-1], GROUPS[1:]):
        if begin > DIRECT:
            quarters, stored[0] = lax.optimization_barrier((quarters, stored[0]))
        group = quarters[begin:end]
        if begin < DIRECT:
            group = from_everyone(group, "fs")
        else:
            group = lax.all_gather(group, "fs", axis=0)
        for layer in range(begin, end):
            stored[layer] = group
    for layer in range(layer_total):
        place = layer - max(begin for begin in GROUPS if begin <= layer)
        fetch = layer in GROUPS and layer >= DIRECT
        if fetch:
            group, everything = lax.optimization_barrier((stored[layer], everything))
            for later in range(layer, layer_total):
                if stored[later] is stored[layer] and later != layer:
                    stored[later] = group
            stored[layer] = group
        weights = stored[layer]
        if fetch:
            weights = pltpu.with_memory_space_constraint(weights, pltpu.HBM)
        own, copies = apply_layer(layer, place, fetch, everything, own, weights, tables)
        everything = exchange(copies, "tp")
    square = everything.astype(jnp.float32)
    row_total = jnp.sum(jnp.sum(square * square, axis=0), axis=1, keepdims=True)
    inv_rms = lax.rsqrt(row_total / model_width + epsilon)
    normalized = own.astype(jnp.float32) * inv_rms * closing_norm_gain[None, :]
    return normalized.astype(jnp.bfloat16)[None]


def solution(mesh):
    placed = (
        P("pp", "fs", "tp"),
        P("pp", None, "tp"),
        P("pp", None, "tp"),
        P("pp", None, "tp"),
        P("pp", None, "tp"),
        P("pp", None, "tp"),
        P("pp", None, "tp"),
        P("pp", "tp"),
        P("pp", None, "tp"),
        P("pp", "tp"),
        P("tp"),
    )
    return jax.shard_map(
        on_device, mesh=mesh, in_specs=placed, out_specs=P("pp", "fs", "tp"), check_vma=False
    )
```
